32 devices in a mesh: ep: 4 (over y, x), tp: 8 (over z, core).
Axes of the slice: x: 2, y: 2, z: 4, core: 2. Of those that a mesh axis runs over, the one named last changes fastest.
Arguments:
- queries: bfloat16 [2, 1024, 4096], P(None, 'tp', 'ep'), may hold values from -6 to 6
- key_vectors: bfloat16 [2, 1024, 4096], P(None, 'tp', 'ep'), may hold values from -6 to 6
- value_vectors: bfloat16 [2, 1024, 4096], P(None, 'tp', 'ep'), may hold values from -12 to 12
- cumulative_gate: float32 [2, 16, 4096], P(None, 'tp'), may hold values from -4096 to 0, as said below
- expert_input: bfloat16 [4096, 2048], P(('ep', 'tp')), may hold values from -6 to 6
- norm_gain: float32 [2048], replicated, may hold values from 0.1 to 1.9
- group_choice: int32 [4096], P(('ep', 'tp')), may hold values from 0 to 3, as said below
- group_weight: float32 [4096], P(('ep', 'tp')), may hold values from 0.3 to 1
- expert_logits: float32 [4096, 2], P(('ep', 'tp')), may hold values from -6 to 6
- gate_weight: bfloat16 [8, 2048, 2048], P('ep', 'tp'), may hold values from -0.125 to 0.125
- up_weight: bfloat16 [8, 2048, 2048], P('ep', 'tp'), may hold values from -0.125 to 0.125
- down_weight: bfloat16 [8, 2048, 2048], P('ep', 'tp'), may hold values from -0.25 to 0.25
Outputs:
- attention: bfloat16 [2, 1024, 4096], P(None, 'tp', 'ep')
- expert_output: bfloat16 [4096, 2048], P(('ep', 'tp'))
The draws below stay inside these ranges and needn't reach their ends.
Inputs may be any that keep to these rules, and one draw needn't show every extreme that they name: `cumulative_gate`: each row is non-increasing along positions. `group_choice`: in each aligned block of 128 rows (the rows of one device) no group is named more than 40 times, and one group is named exactly 40 times in every block.
All inputs are finite; a program needn't handle non-finite values.
Results may differ from the reference program's by a relative error of at most 0.017.
Values may be sent and summed in bfloat16 or wider, within the bound.
A program may use at most 128 MiB of HBM per device.

```python
import math
import jax
import jax.numpy as jnp
from jax import lax

D = 2048
HEADS = 16
HEAD = 64
HD = 1024
FE = 2048
EPG = 2
STRAND_TOTAL = 2
SEG = 1024
STRAND_SPAN = 4096
TOK_DEV = 128
MOE_TOKENS = 4096
GROUPS = 4
EXPERTS = 8
CAP = 40
N_TP = 8


def draw_queries(key, part):
    rows = jnp.clip(1.6 * jax.random.normal(jax.random.fold_in(key, 11), (STRAND_TOTAL, STRAND_SPAN, HD), jnp.float32), -6.0, 6.0)
    return jnp.transpose(rows, (0, 2, 1)).astype(jnp.bfloat16)


def draw_key_vectors(key, part):
    rows = jnp.clip(1.6 * jax.random.normal(jax.random.fold_in(key, 12), (STRAND_TOTAL, STRAND_SPAN, HD), jnp.float32), -6.0, 6.0)
    return jnp.transpose(rows, (0, 2, 1)).astype(jnp.bfloat16)


def draw_cumulative_gate(key, part):
    order = jax.random.permutation(jax.random.fold_in(key, 21), HEADS).astype(jnp.int32)
    fast_span = jnp.exp(jax.random.uniform(jax.random.fold_in(key, 23), (STRAND_TOTAL, HEADS), jnp.float32, math.log(30.0), math.log(100.0)))
    slow = order[None, :] < HEADS // 2
    slow_total = jnp.exp(jax.random.uniform(jax.random.fold_in(key, 22), (STRAND_TOTAL, HEADS), jnp.float32, math.log(0.25), math.log(0.8)))
    rate = jnp.where(slow, slow_total / STRAND_SPAN, 1.0 / fast_span)
    block_factor = jnp.exp(jax.random.uniform(jax.random.fold_in(key, 24), (STRAND_TOTAL, 1, STRAND_SPAN // SEG), jnp.float32, math.log(0.5), math.log(2.0)))
    block_factor = jnp.repeat(block_factor, SEG, axis=2)
    jitter = jax.random.uniform(jax.random.fold_in(key, 25), (STRAND_TOTAL, HEADS, STRAND_SPAN), jnp.float32, 0.1, 1.9)
    pass_tally = -rate[:, :, None] * block_factor * jitter
    stretch_shift = jax.random.randint(jax.random.fold_in(key, 26), (STRAND_TOTAL, 2), 1, STRAND_SPAN).astype(jnp.int32)
    stretch_width = jax.random.uniform(jax.random.fold_in(key, 27), (STRAND_TOTAL, 2), jnp.float32, 0.22, 0.69)
    strand_number = jnp.arange(STRAND_TOTAL, dtype=jnp.int32)[:, None]
    stretch_table = jnp.zeros((STRAND_TOTAL, STRAND_SPAN), jnp.float32).at[strand_number, stretch_shift].add(stretch_width)
    pass_tally = pass_tally - stretch_table[:, None, :]
    return jnp.cumsum(pass_tally, axis=2).astype(jnp.float32)


def draw_group_choice(key, part):
    block_total = MOE_TOKENS // TOK_DEV
    pool_size = GROUPS * CAP
    full_group = jax.random.randint(jax.random.fold_in(key, 31), (), 0, GROUPS).astype(jnp.int32)
    owner = (jnp.arange(pool_size, dtype=jnp.int32) // CAP).astype(jnp.int32)

    def one_block(block_index):
        block_key = jax.random.fold_in(key, 1000 + block_index)
        ranked = jax.random.permutation(jax.random.fold_in(block_key, 1), pool_size).astype(jnp.int32)
        priority = jnp.where(owner == full_group, ranked - pool_size, ranked)
        picked = owner[jnp.argsort(priority)[:TOK_DEV]]
        shuffle = jax.random.permutation(jax.random.fold_in(block_key, 2), TOK_DEV)
        return picked[shuffle]
    return jax.vmap(one_block)(jnp.arange(block_total, dtype=jnp.int32)).reshape(MOE_TOKENS).astype(jnp.int32)


def steps_of(stream_key, extent, pieces, smallest, high):
    gain, own = 1.0, jax.random.fold_in(stream_key, 6)
    for dim, blocks in pieces:
        draws = jnp.exp(jax.random.uniform(jax.random.fold_in(own, dim), (blocks,), jnp.float32, smallest / len(pieces), high / len(pieces)))
        gain = gain * jnp.repeat(draws, extent[dim] // blocks).reshape([-1 if axis == dim else 1 for axis in range(len(extent))])
    return gain


def gaussian(rng, dims, scale, most, shards=(), kind=jnp.bfloat16):
    factor_of = steps_of(rng, dims, shards, -0.22, 0.18) if shards else 1.0
    drawn = jax.random.normal(rng, dims, jnp.float32) * scale * factor_of
    return jnp.minimum(jnp.maximum(drawn, -most), most).astype(kind)


def setup_inputs(seed: int = 0) -> dict:
    streams_of = jax.random.split(jax.random.key(seed), 13)
    queries = draw_queries(jax.random.fold_in(streams_of[12], 71), 0)
    key_vectors = draw_key_vectors(jax.random.fold_in(streams_of[12], 71), 0)
    value_vectors = gaussian(streams_of[2], (STRAND_TOTAL, HD, STRAND_SPAN), 2.0, 12.0, ((1, 8), (2, 4)))
    cumulative_gate = draw_cumulative_gate(jax.random.fold_in(streams_of[12], 71), 0)
    expert_input = gaussian(streams_of[4], (MOE_TOKENS, D), 1.0, 6.0, ((0, 32),))
    norm_gain = jnp.clip(1.0 + 0.18 * jax.random.normal(streams_of[5], (D,), jnp.float32), 0.1, 1.9)
    group_choice = draw_group_choice(jax.random.fold_in(streams_of[12], 71), 0)
    group_weight = jnp.clip(jnp.exp(math.log(1.0) - 1.2039728 * jax.random.uniform(streams_of[7], (MOE_TOKENS,), jnp.float32) ** steps_of(streams_of[7], (MOE_TOKENS,), ((0, 32),), -0.2, 0.2)), 0.3, 1.0)
    expert_logits = gaussian(streams_of[8], (MOE_TOKENS, EPG), 1.5, 6.0, ((0, 32),), jnp.float32)
    gate_weight = gaussian(streams_of[9], (EXPERTS, FE, D), D ** -0.5, 0.125, ((0, 4), (1, 8)))
    up_weight = gaussian(streams_of[10], (EXPERTS, FE, D), D ** -0.5, 0.125, ((0, 4), (1, 8)))
    down_weight = gaussian(streams_of[11], (EXPERTS, FE, D), (FE // 4) ** -0.5, 0.25, ((0, 4), (1, 8)))
    return {"queries": queries, "key_vectors": key_vectors, "value_vectors": value_vectors, "cumulative_gate": cumulative_gate, "expert_input": expert_input, "norm_gain": norm_gain, "group_choice": group_choice, "group_weight": group_weight, "expert_logits": expert_logits, "gate_weight": gate_weight, "up_weight": up_weight, "down_weight": down_weight}


neg_fill = -1e+30
norm_eps = 1e-06

def head_attention(queries, key_vectors, value_vectors, cumulative_gate):
    query_rows = jnp.transpose(queries, (0, 2, 1))
    key_rows = jnp.transpose(key_vectors, (0, 2, 1))
    value_rows = jnp.transpose(value_vectors, (0, 2, 1))
    block_len = min(512, STRAND_SPAN)
    block_count = STRAND_SPAN // block_len
    score_scale = 1.0 / math.sqrt(HEAD)
    zero_index = jnp.zeros((), jnp.int32)
    key_positions = jnp.arange(STRAND_SPAN, dtype=jnp.int32)

    def one_pair(pair_index):
        strand_number = (pair_index // HEADS).astype(jnp.int32)
        head_index = (pair_index % HEADS).astype(jnp.int32)
        column = (head_index * HEAD).astype(jnp.int32)
        query_head = lax.dynamic_slice(query_rows, (strand_number, zero_index, column), (1, STRAND_SPAN, HEAD))[0]
        key_head = lax.dynamic_slice(key_rows, (strand_number, zero_index, column), (1, STRAND_SPAN, HEAD))[0]
        value_head = lax.dynamic_slice(value_rows, (strand_number, zero_index, column), (1, STRAND_SPAN, HEAD))[0]
        gate_head = lax.dynamic_slice(cumulative_gate, (strand_number, head_index, zero_index), (1, 1, STRAND_SPAN))[0, 0]

        def one_block(block_index):
            block_start = (block_index * block_len).astype(jnp.int32)
            query_block = lax.dynamic_slice_in_dim(query_head, block_start, block_len, 0)
            query_gate = lax.dynamic_slice_in_dim(gate_head, block_start, block_len, 0)
            scores = jnp.dot(query_block, key_head.T, preferred_element_type=jnp.float32) * score_scale
            scores = scores + (query_gate[:, None] - gate_head[None, :])
            query_positions = block_start + jnp.arange(block_len, dtype=jnp.int32)
            allowed = key_positions[None, :] <= query_positions[:, None]
            scores = jnp.where(allowed, scores, neg_fill)
            peak = lax.optimization_barrier(jnp.max(scores, axis=1, keepdims=True))
            expo = jnp.where(allowed, jnp.exp(scores - peak), 0.0)
            total = lax.optimization_barrier(jnp.sum(expo, axis=1, keepdims=True))
            mixed = jnp.dot(expo.astype(jnp.bfloat16), value_head, preferred_element_type=jnp.float32) / total
            return mixed.astype(jnp.bfloat16)
        return lax.map(one_block, jnp.arange(block_count, dtype=jnp.int32)).reshape(STRAND_SPAN, HEAD)
    heads_out = lax.map(one_pair, jnp.arange(STRAND_TOTAL * HEADS, dtype=jnp.int32))
    heads_out = heads_out.reshape(STRAND_TOTAL, HEADS, STRAND_SPAN, HEAD)
    return jnp.transpose(heads_out, (0, 1, 3, 2)).reshape(STRAND_TOTAL, HD, STRAND_SPAN)

def expert_mixture(expert_input, norm_gain, group_choice, group_weight, expert_logits, gate_weight, up_weight, down_weight):
    token_float = expert_input.astype(jnp.float32)
    normed = (token_float * lax.rsqrt(lax.optimization_barrier(jnp.mean(token_float * token_float, axis=1, keepdims=True)) + norm_eps) * norm_gain).astype(jnp.bfloat16)
    routing = (group_weight[:, None] * jax.nn.softmax(expert_logits, axis=1)).astype(jnp.bfloat16)
    block_total = MOE_TOKENS // TOK_DEV
    chosen = group_choice.reshape(block_total, TOK_DEV)
    member = (chosen[:, :, None] == jnp.arange(GROUPS, dtype=jnp.int32)[None, None, :]).astype(jnp.int32)
    before = jnp.cumsum(member, axis=1) - member
    slot_index = lax.optimization_barrier(jnp.sum(before * member, axis=2))
    block_ids = jnp.arange(block_total, dtype=jnp.int32)[:, None]
    flat_slot = ((chosen * block_total + block_ids) * CAP + slot_index).reshape(MOE_TOKENS).astype(jnp.int32)
    row_total = block_total * CAP
    row_buffer = jnp.zeros((GROUPS * row_total, D), jnp.bfloat16).at[flat_slot].set(normed).reshape(GROUPS, row_total, D)
    route_buffer = jnp.zeros((GROUPS * row_total, EPG), jnp.bfloat16).at[flat_slot].set(routing).reshape(GROUPS, row_total, EPG)
    hidden_width = FE // N_TP

    def one_group(group_index):
        group_rows = lax.optimization_barrier(row_buffer[group_index]).astype(jnp.float32)
        group_route = lax.optimization_barrier(route_buffer[group_index]).astype(jnp.float32)
        first_expert = (group_index * EPG).astype(jnp.int32)
        gate_block = lax.dynamic_slice_in_dim(gate_weight, first_expert, EPG, 0).astype(jnp.float32)
        up_block = lax.dynamic_slice_in_dim(up_weight, first_expert, EPG, 0).astype(jnp.float32)
        down_block = lax.dynamic_slice_in_dim(down_weight, first_expert, EPG, 0).astype(jnp.float32)
        gate_act = jnp.einsum('rd,efd->ref', group_rows, gate_block)
        up_act = jnp.einsum('rd,efd->ref', group_rows, up_block)
        hidden = (jax.nn.silu(gate_act) * up_act * group_route[:, :, None]).astype(jnp.bfloat16)
        hidden = lax.optimization_barrier(hidden).astype(jnp.float32).reshape(row_total, EPG, N_TP, hidden_width)
        partial_sums = jnp.einsum('rejf,ejfd->rjd', hidden, down_block.reshape(EPG, N_TP, hidden_width, D))
        partial_sums = lax.optimization_barrier(partial_sums.astype(jnp.bfloat16)).astype(jnp.float32)
        return lax.optimization_barrier(jnp.sum(partial_sums, axis=1)).astype(jnp.bfloat16)
    group_out = lax.map(one_group, jnp.arange(GROUPS, dtype=jnp.int32))
    return group_out.reshape(GROUPS * row_total, D)[flat_slot]

def reference(queries, key_vectors, value_vectors, cumulative_gate, expert_input, norm_gain, group_choice, group_weight, expert_logits, gate_weight, up_weight, down_weight):
    attention = head_attention(queries, key_vectors, value_vectors, cumulative_gate)
    expert_output = expert_mixture(expert_input, norm_gain, group_choice, group_weight, expert_logits, gate_weight, up_weight, down_weight)
    return (attention, expert_output)
```

```python
from functools import partial
import math

import jax
import jax.numpy as jnp
from jax import lax
from jax.experimental import pallas as pl
from jax.experimental.pallas import tpu as pltpu
from jax.sharding import PartitionSpec as P

neg_fill = -1e30
norm_eps = 1e-06


def partner(x, axis, distance):
    return lax.ppermute(x, axis, [(i, i ^ 1 << distance) for i in range(lax.axis_size(axis))])


def unchanged(running):
    return running


def attend(queries, key_vectors, value_vectors, cumulative_gate):
    seq_count, feat_width, seg_len = queries.shape
    heads_here = cumulative_gate.shape[1]
    head_dim = feat_width // heads_here
    half_len = seg_len // 2
    ep_size = lax.axis_size("ep")
    ep_rank = lax.axis_index("ep")
    score_scale = 1.0 / math.sqrt(head_dim)
    query_grid = queries.reshape(seq_count, heads_here, head_dim, seg_len)
    early_half = query_grid[:, :, :, :half_len]
    later_half = query_grid[:, :, :, half_len:]
    early_start = ep_rank * seg_len
    for bit_index in range(ep_size.bit_length() - 1):
        later_half = partner(later_half, "ep", bit_index)
    later_start = (ep_size - 1 - ep_rank) * seg_len + half_len
    halves = ((early_half, early_start), (later_half, later_start))
    query_gates = [
        lax.dynamic_slice_in_dim(cumulative_gate, early_start, half_len, 2),
        lax.dynamic_slice_in_dim(cumulative_gate, later_start, half_len, 2),
    ]

    def absorb(running, key_block, value_block, gate_block, key_start, half_index):
        query_block, query_start = halves[half_index]
        peak_old, total_old, acc_old = running
        scores = (
            jnp.einsum(
                "shdq,shdk->shqk", query_block, key_block, preferred_element_type=jnp.float32
            )
            * score_scale
        )
        scores = scores + query_gates[half_index][:, :, :, None] - gate_block[:, :, None, :]
        query_pos = query_start + jnp.arange(half_len, dtype=jnp.int32)
        key_pos = key_start + jnp.arange(key_block.shape[3], dtype=jnp.int32)
        allowed = key_pos[None, :] <= query_pos[:, None]
        scores = jnp.where(allowed, scores, neg_fill)
        peak_new = jnp.maximum(peak_old, jnp.max(scores, axis=3))
        shrink = jnp.exp(peak_old - peak_new)
        weights = jnp.where(allowed, jnp.exp(scores - peak_new[:, :, :, None]), 0.0)
        total_new = total_old * shrink + jnp.sum(weights, axis=3)
        acc_new = acc_old * shrink[:, :, None, :] + jnp.einsum(
            "shqk,shdk->shdq",
            weights.astype(jnp.bfloat16),
            value_block,
            preferred_element_type=jnp.float32,
        )
        return (peak_new, total_new, acc_new)

    blank_state = (
        jnp.full((seq_count, heads_here, half_len), neg_fill, jnp.float32),
        jnp.zeros((seq_count, heads_here, half_len), jnp.float32),
        jnp.zeros((seq_count, heads_here, head_dim, half_len), jnp.float32),
    )
    key_piece = lax.all_gather(key_vectors, "ep", axis=2, tiled=True)
    value_piece = lax.all_gather(value_vectors, "ep", axis=2, tiled=True)
    length = key_piece.shape[2]
    key_span = math.gcd(length, 1024)

    def visit_block(counter, inner):
        offset = counter * key_span
        key_block = lax.dynamic_slice_in_dim(key_piece, offset, key_span, 2).reshape(
            seq_count, heads_here, head_dim, key_span
        )
        value_block = lax.dynamic_slice_in_dim(value_piece, offset, key_span, 2).reshape(
            seq_count, heads_here, head_dim, key_span
        )
        gate_block = lax.dynamic_slice_in_dim(cumulative_gate, offset, key_span, 2)
        updated = []
        for half_index in range(2):
            last_pos = halves[half_index][1] + half_len - 1
            step_fn = partial(
                absorb,
                key_block=key_block,
                value_block=value_block,
                gate_block=gate_block,
                key_start=offset,
                half_index=half_index,
            )
            updated.append(lax.cond(offset <= last_pos, step_fn, unchanged, inner[half_index]))
        return tuple(updated)

    states = lax.fori_loop(0, length // key_span, visit_block, (blank_state, blank_state))
    outputs = []
    for half_index in range(2):
        acc_final = states[half_index][2]
        total_final = states[half_index][1]
        outputs.append((acc_final / total_final[:, :, None, :]).astype(jnp.bfloat16))
    later_out = outputs[1]
    for bit_index in range(ep_size.bit_length() - 1):
        later_out = partner(later_out, "ep", bit_index)
    return jnp.concatenate([outputs[0], later_out], axis=3).reshape(seq_count, feat_width, seg_len)


def gate_rows(gate, sign, first):
    part_a = gate.astype(jnp.bfloat16).astype(jnp.float32)
    rest = gate - part_a
    part_b = rest.astype(jnp.bfloat16).astype(jnp.float32)
    part_c = rest - part_b
    row = lax.broadcasted_iota(jnp.int32, (16, gate.shape[1]), 0)
    ones = jnp.where((row >= 3 - first) & (row < 6 - first), 1.0, 0.0)
    rows = jnp.where(row == first, sign * part_a, ones)
    rows = jnp.where(row == first + 1, sign * part_b, rows)
    return jnp.where(row == first + 2, sign * part_c, rows)


def attend_pair(head_dim, seg_len, seg_count, load, gate_of, store, keys_t, queries_x, values_x, acc, peak):
    scale = 1.0 / math.sqrt(head_dim)
    chunk = min(256, seg_len)
    depth = head_dim + 16

    def fill(block, _):
        gate = gate_of(block)
        local_gate = gate - gate[:, :1]
        at = pl.multiple_of(block * seg_len, seg_len)
        key_rows = jnp.concatenate(
            [load(1, block).astype(jnp.float32), gate_rows(local_gate, -1.0, 0)], axis=0
        )
        keys_t[pl.ds(at, seg_len), :] = jnp.transpose(key_rows).astype(jnp.bfloat16)
        query_rows = jnp.concatenate(
            [load(0, block).astype(jnp.float32) * scale, gate_rows(local_gate, 1.0, 3)], axis=0
        )
        queries_x[block] = query_rows.astype(jnp.bfloat16)
        values_x[block, :head_dim, :] = load(2, block)
        values_x[block, head_dim:, :] = jnp.ones((16, seg_len), jnp.bfloat16)
        return 0

    lax.fori_loop(0, seg_count, fill, 0)

    def query_step(block, _):
        base = gate_of(block)[:, :1]
        at = pl.multiple_of(block * seg_len, seg_len)
        for c in range(seg_len // chunk):
            cols = slice(c * chunk, (c + 1) * chunk)
            span = (c + 1) * chunk
            scores = jnp.dot(
                keys_t[pl.ds(at, span), :],
                queries_x[block, :, cols],
                preferred_element_type=jnp.float32,
            )
            key_pos = lax.broadcasted_iota(jnp.int32, (span, chunk), 0)
            query_pos = c * chunk + lax.broadcasted_iota(jnp.int32, (span, chunk), 1)
            scores = jnp.where(key_pos <= query_pos, scores, neg_fill)
            top = jnp.max(scores, axis=0, keepdims=True)
            weights = jnp.exp(scores - top).astype(jnp.bfloat16)
            peak[:, cols] = top
            acc[:, cols] = jnp.dot(
                values_x[block, :, :span], weights, preferred_element_type=jnp.float32
            )

        def key_step(key_block, _):
            shift = base - gate_of(key_block)[:, :1]
            key_at = pl.multiple_of(key_block * seg_len, seg_len)
            for c in range(seg_len // chunk):
                cols = slice(c * chunk, (c + 1) * chunk)
                scores = jnp.dot(
                    keys_t[pl.ds(key_at, seg_len), :],
                    queries_x[block, :, cols],
                    preferred_element_type=jnp.float32,
                )
                old = peak[:, cols]
                top = jnp.maximum(old, jnp.max(scores, axis=0, keepdims=True) + shift)
                weights = jnp.exp(scores - (top - shift)).astype(jnp.bfloat16)
                peak[:, cols] = top
                acc[:, cols] = acc[:, cols] * jnp.exp(old - top) + jnp.dot(
                    values_x[key_block], weights, preferred_element_type=jnp.float32
                )
            return 0

        lax.fori_loop(0, block, key_step, 0)
        store(block, (acc[:head_dim, :] / acc[head_dim : head_dim + 1, :]).astype(jnp.bfloat16))
        return 0

    lax.fori_loop(0, seg_count, query_step, 0)


def pair_scratch(head_dim, seg_len, seg_count):
    depth = head_dim + 16
    return [
        pltpu.VMEM((seg_len * seg_count, depth), jnp.bfloat16),
        pltpu.VMEM((seg_count, depth, seg_len), jnp.bfloat16),
        pltpu.VMEM((seg_count, depth, seg_len), jnp.bfloat16),
        pltpu.VMEM((depth, seg_len), jnp.float32),
        pltpu.VMEM((1, seg_len), jnp.float32),
    ]


def attend_by_pair(queries, key_vectors, value_vectors, cumulative_gate):
    seq_count, feat_width, seg_len = queries.shape
    heads_here = cumulative_gate.shape[1]
    head_dim = feat_width // heads_here
    ep_size = lax.axis_size("ep")
    share = seq_count * heads_here // ep_size

    def pairs(x):
        return x.reshape(ep_size, share, 1, head_dim, seg_len)

    sent = jnp.concatenate([pairs(queries), pairs(key_vectors), pairs(value_vectors)], axis=2)
    got = lax.all_to_all(sent, "ep", split_axis=0, concat_axis=0, tiled=True)
    gates = lax.dynamic_slice_in_dim(
        cumulative_gate.reshape(seq_count * heads_here, ep_size, 1, seg_len),
        lax.axis_index("ep") * share,
        share,
        0,
    )

    def kernel(got_ref, gate_ref, out_ref, *scratch):
        for p in range(share):

            def store(block, value):
                out_ref[block, p] = value

            attend_pair(
                head_dim,
                seg_len,
                ep_size,
                lambda which, block: got_ref[block, p, which],
                lambda block: gate_ref[p, block],
                store,
                *scratch,
            )

    work = share * head_dim * (seg_len * ep_size) ** 2 * 8
    out = pl.pallas_call(
        kernel,
        out_shape=jax.ShapeDtypeStruct((ep_size, share, head_dim, seg_len), jnp.bfloat16),
        in_specs=[pl.BlockSpec(memory_space=pltpu.VMEM)] * 2,
        out_specs=pl.BlockSpec(memory_space=pltpu.VMEM),
        scratch_shapes=pair_scratch(head_dim, seg_len, ep_size),
        cost_estimate=pl.CostEstimate(flops=work, bytes_accessed=2 << 20, transcendentals=0),
        name="attend_by_pair",
    )(got, gates)
    back = lax.all_to_all(out, "ep", split_axis=0, concat_axis=0, tiled=True)
    return back.reshape(seq_count, feat_width, seg_len)


def expert_hidden(row_block, route_block, gate_weight, up_weight):
    gate_act = jnp.einsum("rd,efd->ref", row_block, gate_weight, preferred_element_type=jnp.float32)
    up_act = jnp.einsum("rd,efd->ref", row_block, up_weight, preferred_element_type=jnp.float32)
    return (jax.nn.silu(gate_act) * up_act * route_block.astype(jnp.float32)[:, :, None]).astype(
        jnp.bfloat16
    )


def mixture(
    expert_input,
    norm_gain,
    group_choice,
    group_weight,
    expert_logits,
    gate_weight,
    up_weight,
    down_weight,
):
    tok_rows, model_dim = expert_input.shape
    group_size = gate_weight.shape[0]
    ep_size = lax.axis_size("ep")
    capacity = 5 * tok_rows // (4 * ep_size)
    token_float = expert_input.astype(jnp.float32)
    normed = (
        token_float
        * lax.rsqrt(jnp.mean(token_float * token_float, axis=1, keepdims=True) + norm_eps)
        * norm_gain
    ).astype(jnp.bfloat16)
    routing = (group_weight[:, None] * jax.nn.softmax(expert_logits, axis=1)).astype(jnp.bfloat16)
    member = (group_choice[:, None] == jnp.arange(ep_size, dtype=jnp.int32)[None, :]).astype(
        jnp.int32
    )
    before = jnp.cumsum(member, axis=0) - member
    slot_index = jnp.sum(before * member, axis=1)
    flat_slot = group_choice * capacity + slot_index
    places = (
        flat_slot[None, :] == jnp.arange(ep_size * capacity, dtype=jnp.int32)[:, None]
    ).astype(jnp.bfloat16)
    payload = jnp.concatenate(
        [normed, routing, jnp.zeros((tok_rows, 128 - group_size), jnp.bfloat16)], axis=1
    )
    outgoing = (
        jnp.dot(places, payload, preferred_element_type=jnp.float32)
        .astype(jnp.bfloat16)
        .reshape(ep_size, capacity, model_dim + 128)
    )
    arrived = lax.all_to_all(outgoing, "ep", split_axis=0, concat_axis=0, tiled=True)
    local_rows = arrived.reshape(ep_size * capacity, model_dim + 128)
    gathered = lax.all_gather(local_rows, "tp", axis=0, tiled=True)
    gathered_rows = gathered[:, :model_dim]
    gathered_route = gathered[:, model_dim : model_dim + group_size]
    hidden = expert_hidden(gathered_rows, gathered_route, gate_weight, up_weight)
    summed = lax.psum_scatter(
        jnp.einsum("ref,efd->rd", hidden, down_weight, preferred_element_type=jnp.float32).astype(
            jnp.bfloat16
        ),
        "tp",
        scatter_dimension=0,
        tiled=True,
    )
    returned = lax.all_to_all(
        summed.reshape(ep_size, capacity, model_dim), "ep", split_axis=0, concat_axis=0, tiled=True
    )
    returned_flat = returned.reshape(ep_size * capacity, model_dim)
    return jnp.einsum(
        "pt,pd->td", places, returned_flat, preferred_element_type=jnp.float32
    ).astype(jnp.bfloat16)


def local(
    queries,
    key_vectors,
    value_vectors,
    cumulative_gate,
    expert_input,
    norm_gain,
    group_choice,
    group_weight,
    expert_logits,
    gate_weight,
    up_weight,
    down_weight,
):
    pair_count = queries.shape[0] * cumulative_gate.shape[1]
    way = attend_by_pair if pair_count % lax.axis_size("ep") == 0 else attend
    attention = way(queries, key_vectors, value_vectors, cumulative_gate)
    expert_output = mixture(
        expert_input,
        norm_gain,
        group_choice,
        group_weight,
        expert_logits,
        gate_weight,
        up_weight,
        down_weight,
    )
    return (attention, expert_output)


def solution(mesh):
    return jax.shard_map(
        local,
        mesh=mesh,
        in_specs=(
            P(None, "tp", "ep"),
            P(None, "tp", "ep"),
            P(None, "tp", "ep"),
            P(None, "tp", None),
            P(("ep", "tp"), None),
            P(),
            P(("ep", "tp")),
            P(("ep", "tp")),
            P(("ep", "tp"), None),
            P("ep", "tp", None),
            P("ep", "tp", None),
            P("ep", "tp", None),
        ),
        out_specs=(P(None, "tp", "ep"), P(("ep", "tp"), None)),
        check_vma=False,
    )
```

```python
from functools import partial
import math

import jax
import jax.numpy as jnp
from jax import lax
from jax.experimental import pallas as pl
from jax.experimental.pallas import tpu as pltpu
from jax.sharding import PartitionSpec as P

neg_fill = -1e30
norm_eps = 1e-06


def partner(x, axis, distance):
    return lax.ppermute(x, axis, [(i, i ^ 1 << distance) for i in range(lax.axis_size(axis))])


def unchanged(running):
    return running


def attend(queries, key_vectors, value_vectors, cumulative_gate):
    seq_count, feat_width, seg_len = queries.shape
    heads_here = cumulative_gate.shape[1]
    head_dim = feat_width // heads_here
    half_len = seg_len // 2
    ep_size = lax.axis_size("ep")
    ep_rank = lax.axis_index("ep")
    score_scale = 1.0 / math.sqrt(head_dim)
    query_grid = queries.reshape(seq_count, heads_here, head_dim, seg_len)
    early_half = query_grid[:, :, :, :half_len]
    later_half = query_grid[:, :, :, half_len:]
    early_start = ep_rank * seg_len
    for bit_index in range(ep_size.bit_length() - 1):
        later_half = partner(later_half, "ep", bit_index)
    later_start = (ep_size - 1 - ep_rank) * seg_len + half_len
    halves = ((early_half, early_start), (later_half, later_start))
    query_gates = [
        lax.dynamic_slice_in_dim(cumulative_gate, early_start, half_len, 2),
        lax.dynamic_slice_in_dim(cumulative_gate, later_start, half_len, 2),
    ]

    def absorb(running, key_block, value_block, gate_block, key_start, half_index):
        query_block, query_start = halves[half_index]
        peak_old, total_old, acc_old = running
        scores = (
            jnp.einsum(
                "shdq,shdk->shqk", query_block, key_block, preferred_element_type=jnp.float32
            )
            * score_scale
        )
        scores = scores + query_gates[half_index][:, :, :, None] - gate_block[:, :, None, :]
        query_pos = query_start + jnp.arange(half_len, dtype=jnp.int32)
        key_pos = key_start + jnp.arange(key_block.shape[3], dtype=jnp.int32)
        allowed = key_pos[None, :] <= query_pos[:, None]
        scores = jnp.where(allowed, scores, neg_fill)
        peak_new = jnp.maximum(peak_old, jnp.max(scores, axis=3))
        shrink = jnp.exp(peak_old - peak_new)
        weights = jnp.where(allowed, jnp.exp(scores - peak_new[:, :, :, None]), 0.0)
        total_new = total_old * shrink + jnp.sum(weights, axis=3)
        acc_new = acc_old * shrink[:, :, None, :] + jnp.einsum(
            "shqk,shdk->shdq",
            weights.astype(jnp.bfloat16),
            value_block,
            preferred_element_type=jnp.float32,
        )
        return (peak_new, total_new, acc_new)

    blank_state = (
        jnp.full((seq_count, heads_here, half_len), neg_fill, jnp.float32),
        jnp.zeros((seq_count, heads_here, half_len), jnp.float32),
        jnp.zeros((seq_count, heads_here, head_dim, half_len), jnp.float32),
    )
    key_piece = lax.all_gather(key_vectors, "ep", axis=2, tiled=True)
    value_piece = lax.all_gather(value_vectors, "ep", axis=2, tiled=True)
    length = key_piece.shape[2]
    key_span = math.gcd(length, 1024)

    def visit_block(counter, inner):
        offset = counter * key_span
        key_block = lax.dynamic_slice_in_dim(key_piece, offset, key_span, 2).reshape(
            seq_count, heads_here, head_dim, key_span
        )
        value_block = lax.dynamic_slice_in_dim(value_piece, offset, key_span, 2).reshape(
            seq_count, heads_here, head_dim, key_span
        )
        gate_block = lax.dynamic_slice_in_dim(cumulative_gate, offset, key_span, 2)
        updated = []
        for half_index in range(2):
            last_pos = halves[half_index][1] + half_len - 1
            step_fn = partial(
                absorb,
                key_block=key_block,
                value_block=value_block,
                gate_block=gate_block,
                key_start=offset,
                half_index=half_index,
            )
            updated.append(lax.cond(offset <= last_pos, step_fn, unchanged, inner[half_index]))
        return tuple(updated)

    states = lax.fori_loop(0, length // key_span, visit_block, (blank_state, blank_state))
    outputs = []
    for half_index in range(2):
        acc_final = states[half_index][2]
        total_final = states[half_index][1]
        outputs.append((acc_final / total_final[:, :, None, :]).astype(jnp.bfloat16))
    later_out = outputs[1]
    for bit_index in range(ep_size.bit_length() - 1):
        later_out = partner(later_out, "ep", bit_index)
    return jnp.concatenate([outputs[0], later_out], axis=3).reshape(seq_count, feat_width, seg_len)


def gate_rows(gate, sign, first):
    part_a = gate.astype(jnp.bfloat16).astype(jnp.float32)
    rest = gate - part_a
    part_b = rest.astype(jnp.bfloat16).astype(jnp.float32)
    part_c = rest - part_b
    row = lax.broadcasted_iota(jnp.int32, (16, gate.shape[1]), 0)
    ones = jnp.where((row >= 3 - first) & (row < 6 - first), 1.0, 0.0)
    rows = jnp.where(row == first, sign * part_a, ones)
    rows = jnp.where(row == first + 1, sign * part_b, rows)
    return jnp.where(row == first + 2, sign * part_c, rows)


def attend_pair(head_dim, seg_len, seg_count, load, gate_of, store, keys_t, queries_x, values_x, acc, peak):
    scale = 1.0 / math.sqrt(head_dim)
    chunk = min(256, seg_len)
    depth = head_dim + 16

    def fill(block, _):
        gate = gate_of(block)
        local_gate = gate - gate[:, :1]
        at = pl.multiple_of(block * seg_len, seg_len)
        key_rows = jnp.concatenate(
            [load(1, block).astype(jnp.float32), gate_rows(local_gate, -1.0, 0)], axis=0
        )
        keys_t[pl.ds(at, seg_len), :] = jnp.transpose(key_rows).astype(jnp.bfloat16)
        query_rows = jnp.concatenate(
            [load(0, block).astype(jnp.float32) * scale, gate_rows(local_gate, 1.0, 3)], axis=0
        )
        queries_x[block] = query_rows.astype(jnp.bfloat16)
        values_x[block, :head_dim, :] = load(2, block)
        values_x[block, head_dim:, :] = jnp.ones((16, seg_len), jnp.bfloat16)
        return 0

    lax.fori_loop(0, seg_count, fill, 0)

    def query_step(block, _):
        base = gate_of(block)[:, :1]
        at = pl.multiple_of(block * seg_len, seg_len)
        for c in range(seg_len // chunk):
            cols = slice(c * chunk, (c + 1) * chunk)
            span = (c + 1) * chunk
            scores = jnp.dot(
                keys_t[pl.ds(at, span), :],
                queries_x[block, :, cols],
                preferred_element_type=jnp.float32,
            )
            key_pos = lax.broadcasted_iota(jnp.int32, (span, chunk), 0)
            query_pos = c * chunk + lax.broadcasted_iota(jnp.int32, (span, chunk), 1)
            scores = jnp.where(key_pos <= query_pos, scores, neg_fill)
            top = jnp.max(scores, axis=0, keepdims=True)
            weights = jnp.exp(scores - top).astype(jnp.bfloat16)
            peak[:, cols] = top
            acc[:, cols] = jnp.dot(
                values_x[block, :, :span], weights, preferred_element_type=jnp.float32
            )

        def key_step(key_block, _):
            shift = base - gate_of(key_block)[:, :1]
            key_at = pl.multiple_of(key_block * seg_len, seg_len)
            for c in range(seg_len // chunk):
                cols = slice(c * chunk, (c + 1) * chunk)
                scores = jnp.dot(
                    keys_t[pl.ds(key_at, seg_len), :],
                    queries_x[block, :, cols],
                    preferred_element_type=jnp.float32,
                )
                old = peak[:, cols]
                top = jnp.maximum(old, jnp.max(scores, axis=0, keepdims=True) + shift)
                weights = jnp.exp(scores - (top - shift)).astype(jnp.bfloat16)
                peak[:, cols] = top
                acc[:, cols] = acc[:, cols] * jnp.exp(old - top) + jnp.dot(
                    values_x[key_block], weights, preferred_element_type=jnp.float32
                )
            return 0

        lax.fori_loop(0, block, key_step, 0)
        store(block, (acc[:head_dim, :] / acc[head_dim : head_dim + 1, :]).astype(jnp.bfloat16))
        return 0

    lax.fori_loop(0, seg_count, query_step, 0)


def pair_scratch(head_dim, seg_len, seg_count):
    depth = head_dim + 16
    return [
        pltpu.VMEM((seg_len * seg_count, depth), jnp.bfloat16),
        pltpu.VMEM((seg_count, depth, seg_len), jnp.bfloat16),
        pltpu.VMEM((seg_count, depth, seg_len), jnp.bfloat16),
        pltpu.VMEM((depth, seg_len), jnp.float32),
        pltpu.VMEM((1, seg_len), jnp.float32),
    ]


def attend_by_pair(queries, key_vectors, value_vectors, cumulative_gate):
    seq_count, feat_width, seg_len = queries.shape
    heads_here = cumulative_gate.shape[1]
    head_dim = feat_width // heads_here
    ep_size = lax.axis_size("ep")
    share = seq_count * heads_here // ep_size

    def pairs(x):
        return x.reshape(ep_size, share, 1, head_dim, seg_len)

    sent = jnp.concatenate([pairs(queries), pairs(key_vectors), pairs(value_vectors)], axis=2)
    got = lax.all_to_all(sent, "ep", split_axis=0, concat_axis=0, tiled=True)
    gates = lax.dynamic_slice_in_dim(
        cumulative_gate.reshape(seq_count * heads_here, ep_size, 1, seg_len),
        lax.axis_index("ep") * share,
        share,
        0,
    )

    def kernel(got_ref, gate_ref, out_ref, *scratch):
        for p in range(share):

            def store(block, value):
                out_ref[block, p] = value

            attend_pair(
                head_dim,
                seg_len,
                ep_size,
                lambda which, block: got_ref[block, p, which],
                lambda block: gate_ref[p, block],
                store,
                *scratch,
            )

    work = share * head_dim * (seg_len * ep_size) ** 2 * 24
    out = pl.pallas_call(
        kernel,
        out_shape=jax.ShapeDtypeStruct((ep_size, share, head_dim, seg_len), jnp.bfloat16),
        in_specs=[pl.BlockSpec(memory_space=pltpu.VMEM)] * 2,
        out_specs=pl.BlockSpec(memory_space=pltpu.VMEM),
        scratch_shapes=pair_scratch(head_dim, seg_len, ep_size),
        cost_estimate=pl.CostEstimate(flops=work, bytes_accessed=2 << 20, transcendentals=0),
        name="attend_by_pair",
    )(got, gates)
    back = lax.all_to_all(out, "ep", split_axis=0, concat_axis=0, tiled=True)
    return back.reshape(seq_count, feat_width, seg_len)


def experts_on_line(gathered, gate_weight, up_weight, down_weight):
    n_tp, rows, width = gathered.shape
    group_size, hidden_width, model_dim = gate_weight.shape
    chips = n_tp // 2
    last = chips - 1

    def kernel(
        rows_ref, gate_ref, up_ref, down_ref, out_ref,
        part, sums, pair_out, pair_in, line_out, line_in,
        pair_ss, pair_rs, line_ss, line_rs,
    ):
        tp = lax.axis_index("tp")
        z = tp // 2
        core = tp % 2
        sibling = z * 2 + 1 - core
        barrier = pltpu.get_barrier_semaphore()

        def greet(other):
            pl.semaphore_signal(
                barrier, inc=1, device_id={"tp": other}, device_id_type=pl.DeviceIdType.MESH
            )

        greet(sibling)

        @pl.when(z > 0)
        def _():
            greet(tp - 2)

        @pl.when(z < last)
        def _():
            greet(tp + 2)

        inside = (z > 0) & (z < last)

        @pl.when(inside)
        def _():
            pl.semaphore_wait(barrier, 3)

        @pl.when(jnp.logical_not(inside))
        def _():
            pl.semaphore_wait(barrier, 2 if last > 0 else 1)

        def pair_copy(t):
            return pltpu.make_async_remote_copy(
                pair_out.at[t], pair_in.at[t], pair_ss.at[t], pair_rs.at[t],
                device_id={"tp": sibling}, device_id_type=pl.DeviceIdType.MESH,
            )

        def line_copy(t, slot, other):
            return pltpu.make_async_remote_copy(
                line_out.at[t], line_in.at[slot], line_ss.at[t], line_rs.at[slot],
                device_id={"tp": other}, device_id_type=pl.DeviceIdType.MESH,
            )

        def send_right(t):
            line_copy(t, t, tp + 2).start()

        def send_left(t):
            @pl.when(t == z - 1)
            def _():
                line_copy(t, chips, tp - 2).start()

            @pl.when(t < z - 1)
            def _():
                line_copy(t, t, tp - 2).start()

        upper = (2 * z) // chips

        def compute(i, _):
            t = (1 - upper) * (last - i) + upper * i
            block = rows_ref[pl.ds(t * 2, 2)].reshape(2 * rows, width)
            tokens = block[:, :model_dim]
            route = block[:, model_dim:].astype(jnp.float32)
            for e in range(group_size):
                nt = (((1,), (1,)), ((), ()))
                gate_act = lax.dot_general(
                    tokens, gate_ref[e], nt, preferred_element_type=jnp.float32
                )
                up_act = lax.dot_general(tokens, up_ref[e], nt, preferred_element_type=jnp.float32)
                hidden = gate_act / (1.0 + jnp.exp(-gate_act)) * up_act * route[:, e : e + 1]
                term = jnp.dot(
                    hidden.astype(jnp.bfloat16), down_ref[e], preferred_element_type=jnp.float32
                ).reshape(2, rows, model_dim)
                if e == 0:
                    part[...] = term
                else:
                    part[...] += term
            pair_out[t] = part[1 - core].astype(jnp.bfloat16)
            copy = pair_copy(t)
            copy.start()
            copy.wait_recv()
            sums[t] = part[core] + pair_in[t].astype(jnp.float32)

            @pl.when((z == 0) & (t > 0))
            def _():
                line_out[t] = sums[t].astype(jnp.bfloat16)
                send_right(t)

            @pl.when((z == last) & (t < last))
            def _():
                line_out[t] = sums[t].astype(jnp.bfloat16)
                send_left(t)

            return 0

        lax.fori_loop(0, chips, compute, 0)

        def pass_on(k, _):
            right_t = last - (k - z)
            left_t = k - (last - z)

            @pl.when((z > 0) & (k >= z) & (right_t > z))
            def _():
                line_copy(right_t, right_t, tp).wait_recv()
                line_out[right_t] = (
                    sums[right_t] + line_in[right_t].astype(jnp.float32)
                ).astype(jnp.bfloat16)
                send_right(right_t)

            @pl.when((z < last) & (left_t >= 0) & (left_t < z))
            def _():
                line_copy(left_t, left_t, tp).wait_recv()
                line_out[left_t] = (
                    sums[left_t] + line_in[left_t].astype(jnp.float32)
                ).astype(jnp.bfloat16)
                send_left(left_t)

            return 0

        lax.fori_loop(1, chips, pass_on, 0)

        @pl.when(z > 0)
        def _():
            line_copy(z, z, tp).wait_recv()
            sums[z] = sums[z] + line_in[z].astype(jnp.float32)

        @pl.when(z < last)
        def _():
            line_copy(z, chips, tp).wait_recv()
            sums[z] = sums[z] + line_in[chips].astype(jnp.float32)

        out_ref[...] = sums[z].astype(jnp.bfloat16)

        def drain(t, _):
            pair_copy(t).wait_send()

            @pl.when(t != z)
            def _():
                line_copy(t, t, tp).wait_send()

            return 0

        lax.fori_loop(0, chips, drain, 0)

    flops = 6 * n_tp * rows * group_size * hidden_width * model_dim
    return pl.pallas_call(
        kernel,
        out_shape=jax.ShapeDtypeStruct((rows, model_dim), jnp.bfloat16),
        in_specs=[pl.BlockSpec(memory_space=pltpu.VMEM)] * 4,
        out_specs=pl.BlockSpec(memory_space=pltpu.VMEM),
        scratch_shapes=[
            pltpu.VMEM((2, rows, model_dim), jnp.float32),
            pltpu.VMEM((chips, rows, model_dim), jnp.float32),
            pltpu.VMEM((chips, rows, model_dim), jnp.bfloat16),
            pltpu.VMEM((chips, rows, model_dim), jnp.bfloat16),
            pltpu.VMEM((chips, rows, model_dim), jnp.bfloat16),
            pltpu.VMEM((chips + 1, rows, model_dim), jnp.bfloat16),
            pltpu.SemaphoreType.DMA((chips,)),
            pltpu.SemaphoreType.DMA((chips,)),
            pltpu.SemaphoreType.DMA((chips,)),
            pltpu.SemaphoreType.DMA((chips + 1,)),
        ],
        compiler_params=pltpu.CompilerParams(
            collective_id=0, has_side_effects=True, vmem_limit_bytes=63 << 20
        ),
        cost_estimate=pl.CostEstimate(flops=4 * flops, bytes_accessed=12 << 20, transcendentals=0),
        name="experts_on_line",
    )(gathered, gate_weight, up_weight, down_weight)


def mixture(
    expert_input,
    norm_gain,
    group_choice,
    group_weight,
    expert_logits,
    gate_weight,
    up_weight,
    down_weight,
):
    tok_rows, model_dim = expert_input.shape
    group_size = gate_weight.shape[0]
    ep_size = lax.axis_size("ep")
    capacity = 5 * tok_rows // (4 * ep_size)
    token_float = expert_input.astype(jnp.float32)
    normed = (
        token_float
        * lax.rsqrt(jnp.mean(token_float * token_float, axis=1, keepdims=True) + norm_eps)
        * norm_gain
    ).astype(jnp.bfloat16)
    routing = (group_weight[:, None] * jax.nn.softmax(expert_logits, axis=1)).astype(jnp.bfloat16)
    member = (group_choice[:, None] == jnp.arange(ep_size, dtype=jnp.int32)[None, :]).astype(
        jnp.int32
    )
    before = jnp.cumsum(member, axis=0) - member
    slot_index = jnp.sum(before * member, axis=1)
    flat_slot = group_choice * capacity + slot_index
    places = (
        flat_slot[None, :] == jnp.arange(ep_size * capacity, dtype=jnp.int32)[:, None]
    ).astype(jnp.bfloat16)
    payload = jnp.concatenate(
        [normed, routing, jnp.zeros((tok_rows, 128 - group_size), jnp.bfloat16)], axis=1
    )
    outgoing = (
        jnp.dot(places, payload, preferred_element_type=jnp.float32)
        .astype(jnp.bfloat16)
        .reshape(ep_size, capacity, model_dim + 128)
    )
    arrived = lax.all_to_all(outgoing, "ep", split_axis=0, concat_axis=0, tiled=True)
    local_rows = arrived.reshape(ep_size * capacity, model_dim + 128)
    gathered = lax.all_gather(local_rows, "tp", axis=0)
    summed = experts_on_line(gathered, gate_weight, up_weight, down_weight)
    returned = lax.all_to_all(
        summed.reshape(ep_size, capacity, model_dim), "ep", split_axis=0, concat_axis=0, tiled=True
    )
    returned_flat = returned.reshape(ep_size * capacity, model_dim)
    return jnp.einsum(
        "pt,pd->td", places, returned_flat, preferred_element_type=jnp.float32
    ).astype(jnp.bfloat16)


def local(
    queries,
    key_vectors,
    value_vectors,
    cumulative_gate,
    expert_input,
    norm_gain,
    group_choice,
    group_weight,
    expert_logits,
    gate_weight,
    up_weight,
    down_weight,
):
    pair_count = queries.shape[0] * cumulative_gate.shape[1]
    way = attend_by_pair if pair_count % lax.axis_size("ep") == 0 else attend
    attention = way(queries, key_vectors, value_vectors, cumulative_gate)
    expert_output = mixture(
        expert_input,
        norm_gain,
        group_choice,
        group_weight,
        expert_logits,
        gate_weight,
        up_weight,
        down_weight,
    )
    return (attention, expert_output)


def solution(mesh):
    return jax.shard_map(
        local,
        mesh=mesh,
        in_specs=(
            P(None, "tp", "ep"),
            P(None, "tp", "ep"),
            P(None, "tp", "ep"),
            P(None, "tp", None),
            P(("ep", "tp"), None),
            P(),
            P(("ep", "tp")),
            P(("ep", "tp")),
            P(("ep", "tp"), None),
            P("ep", "tp", None),
            P("ep", "tp", None),
            P("ep", "tp", None),
        ),
        out_specs=(P(None, "tp", "ep"), P(("ep", "tp"), None)),
        check_vma=False,
    )
```
